32 devices in a mesh: sp: 16 (over z, y, x), tp: 2 (over core).
Axes of the slice: x: 2, y: 2, z: 4, core: 2. Of those that a mesh axis runs over, the one named last changes fastest.
Arguments:
- latent: bfloat16 [4096, 2048], P(('sp', 'tp')), may hold values from -6 to 6
- condition: bfloat16 [2048], P('sp'), may hold values from -6 to 6
- context_condition: bfloat16 [2048], P('sp'), may hold values from -6 to 6
- context: bfloat16 [512, 2048], P('sp'), may hold values from -6 to 6
- w_shift: bfloat16 [2048, 2048], P('sp', 'tp'), may hold values from -0.125 to 0.125
- w_scale: bfloat16 [2048, 2048], P('sp', 'tp'), may hold values from -0.125 to 0.125
- w_gate: bfloat16 [2048, 2048], P('sp', 'tp'), may hold values from -0.125 to 0.125
- pre_gain: float32 [2048], replicated, may hold values from 0.1 to 1.9
- post_gain: float32 [2048], replicated, may hold values from 0.1 to 1.9
- query_gain: float32 [128], replicated, may hold values from 0.1 to 5
- key_gain: float32 [128], replicated, may hold values from 0.1 to 5
- w_query: bfloat16 [2048, 2048], P(None, 'tp'), may hold values from -0.125 to 0.125
- w_key: bfloat16 [2048, 1024], P(None, 'tp'), may hold values from -0.125 to 0.125
- w_value: bfloat16 [2048, 1024], P(None, 'tp'), may hold values from -0.125 to 0.125
- w_out: bfloat16 [2048, 2048], P('tp'), may hold values from -0.125 to 0.125
Outputs:
- updated: bfloat16 [4096, 2048], P(('sp', 'tp'))
The draws below stay inside these ranges and needn't reach their ends.
All inputs are finite; a program needn't handle non-finite values.
Results may differ from the reference program's by a relative error of at most 0.0085.
The reference program's roundings to bfloat16 on the way count: a program that leaves them out, or rounds other values in their place, can miss the bound.
Values may be sent and summed in bfloat16 or wider, within the bound.
A program may use at most 64 MiB of HBM per device.

```python
import math
import jax
import jax.numpy as jnp
from jax import lax

D = 2048
HEADS = 16
KV_HEADS = 8
HEAD_DIM = 128
GRID_W = 64
CTX = 512
TOKENS = 4096
N_TP = 2


def gain_draw(key):
    return 1.0 + 0.18 * jnp.clip(jax.random.normal(key, (HEAD_DIM,), jnp.float32), -4.5, 4.5)


def draw_query_gain(key, part):
    return gain_draw(jax.random.fold_in(key, 11))


def draw_key_gain(key, part):
    return gain_draw(jax.random.fold_in(key, 23))


def block_scale(key, extent, cuts, smallest, top_value):
    factor_of = 1.0
    for position, parts in cuts:
        steps = jax.random.uniform(jax.random.fold_in(jax.random.fold_in(key, 6), position), (parts,), jnp.float32, smallest / len(cuts), top_value / len(cuts))
        factor_of = factor_of * jnp.repeat(jnp.exp(steps), extent[position] // parts).reshape((-1,) + (1,) * (len(extent) - 1 - position))
    return factor_of


def gaussian(key, extent, deviation, bound, cuts=(), held_as=jnp.bfloat16):
    level = block_scale(key, extent, cuts, -0.22, 0.18) if cuts else 1.0
    drawn = jax.random.normal(key, extent, jnp.float32) * deviation * level
    return jnp.minimum(jnp.maximum(drawn, -bound), bound).astype(held_as)


def setup_inputs(seed: int = 0) -> dict:
    arg_keys = jax.random.split(jax.random.key(seed), 16)
    return {
        "latent": gaussian(arg_keys[0], (TOKENS, D), 1.0, 6.0, ((0, 32),)),
        "condition": gaussian(arg_keys[1], (D,), 1.0, 6.0, ((0, 16),)),
        "context_condition": gaussian(arg_keys[2], (D,), 1.0, 6.0, ((0, 16),)),
        "context": gaussian(arg_keys[3], (CTX, D), 1.0, 6.0, ((0, 16),)),
        "w_shift": gaussian(arg_keys[4], (D, D), D ** -0.5, 0.125, ((0, 16), (1, 2))),
        "w_scale": gaussian(arg_keys[5], (D, D), D ** -0.5, 0.125, ((0, 16), (1, 2))),
        "w_gate": gaussian(arg_keys[6], (D, D), D ** -0.5, 0.125, ((0, 16), (1, 2))),
        "pre_gain": jnp.clip(1.0 + 0.18 * jax.random.normal(arg_keys[7], (D,), jnp.float32), 0.1, 1.9),
        "post_gain": jnp.clip(1.0 + 0.18 * jax.random.normal(arg_keys[8], (D,), jnp.float32), 0.1, 1.9),
        "query_gain": draw_query_gain(jax.random.fold_in(arg_keys[15], 71), 0),
        "key_gain": draw_key_gain(jax.random.fold_in(arg_keys[15], 71), 0),
        "w_query": gaussian(arg_keys[11], (D, HEADS * HEAD_DIM), D ** -0.5, 0.125, ((1, 2),)),
        "w_key": gaussian(arg_keys[12], (D, KV_HEADS * HEAD_DIM), D ** -0.5, 0.125, ((1, 2),)),
        "w_value": gaussian(arg_keys[13], (D, KV_HEADS * HEAD_DIM), D ** -0.5, 0.125, ((1, 2),)),
        "w_out": gaussian(arg_keys[14], (HEADS * HEAD_DIM, D), (HEADS * HEAD_DIM) ** -0.5, 0.125, ((0, 2),)),
    }


def rms(values, gain):
    values = values.astype(jnp.float32)
    return values * lax.rsqrt(lax.optimization_barrier(jnp.mean(values * values, axis=-1, keepdims=True)) + 1e-06) * gain

def rotate_grid(values, positions, grid_width):
    head_dim = values.shape[-1]
    half = head_dim // 2
    quarter = head_dim // 4
    freqs = 10000.0 ** (-jnp.arange(0, half, 2).astype(jnp.float32) / half)
    row_pos = (positions // grid_width).astype(jnp.float32)
    col_pos = (positions % grid_width).astype(jnp.float32)
    pieces = []
    for axis_pos, base in ((row_pos, 0), (col_pos, half)):
        angle = axis_pos[:, None, None] * freqs
        cosine = jnp.cos(angle)
        sine = jnp.sin(angle)
        first = values[..., base:base + quarter]
        second = values[..., base + quarter:base + half]
        pieces = pieces + [first * cosine - second * sine, second * cosine + first * sine]
    return jnp.concatenate(pieces, axis=-1)

def reference(latent, condition, context_condition, context, w_shift, w_scale, w_gate, pre_gain, post_gain, query_gain, key_gain, w_query, w_key, w_value, w_out):
    head_dim = HEAD_DIM
    group = HEADS // KV_HEADS
    conds = jax.nn.silu(jnp.stack([condition, context_condition]).astype(jnp.float32)).astype(jnp.bfloat16)
    shift = jnp.dot(conds, w_shift, preferred_element_type=jnp.float32)
    scale = jnp.dot(conds, w_scale, preferred_element_type=jnp.float32)
    gate = jnp.dot(conds, w_gate, preferred_element_type=jnp.float32)
    normed = (rms(latent, pre_gain) * (1.0 + scale[0]) + shift[0]).astype(jnp.bfloat16)
    normed_context = (rms(context, pre_gain) * (1.0 + scale[1]) + shift[1]).astype(jnp.bfloat16)
    positions = jnp.arange(TOKENS).astype(jnp.int32)
    query = jnp.dot(normed, w_query, preferred_element_type=jnp.float32).reshape(TOKENS, HEADS, head_dim)
    query = rotate_grid(rms(query, query_gain), positions, GRID_W).astype(jnp.bfloat16)
    key = jnp.dot(normed, w_key, preferred_element_type=jnp.float32).reshape(TOKENS, KV_HEADS, head_dim)
    key = rotate_grid(rms(key, key_gain), positions, GRID_W).astype(jnp.bfloat16)
    value = jnp.dot(normed, w_value, preferred_element_type=jnp.float32).astype(jnp.bfloat16)
    value = value.reshape(TOKENS, KV_HEADS, head_dim)
    context_key = jnp.dot(normed_context, w_key, preferred_element_type=jnp.float32).reshape(CTX, KV_HEADS, head_dim)
    context_key = rms(context_key, key_gain).astype(jnp.bfloat16)
    context_value = jnp.dot(normed_context, w_value, preferred_element_type=jnp.float32).astype(jnp.bfloat16)
    context_value = context_value.reshape(CTX, KV_HEADS, head_dim)
    all_keys = jnp.concatenate([key, context_key], axis=0).astype(jnp.float32)
    all_values = jnp.concatenate([value, context_value], axis=0).astype(jnp.float32)
    lift = math.log(TOKENS / (4.0 * CTX))
    offsets = jnp.concatenate([jnp.zeros((TOKENS,), jnp.float32), jnp.full((CTX,), lift, jnp.float32)])
    block = 128
    blocked = query.reshape(TOKENS // block, block, KV_HEADS, group, head_dim)

    def one_block(query_block):
        scores = jnp.einsum('tkgd,skd->kgts', query_block.astype(jnp.float32), all_keys) * head_dim ** (-0.5)
        scores = scores + offsets
        largest = lax.optimization_barrier(jnp.max(scores, axis=-1, keepdims=True))
        terms = jnp.exp(scores - largest)
        total = lax.optimization_barrier(jnp.sum(terms, axis=-1))
        rounded = lax.optimization_barrier(terms.astype(jnp.bfloat16)).astype(jnp.float32)
        summed = jnp.einsum('kgts,skd->kgtd', rounded, all_values)
        result = summed / total[..., None]
        return result.transpose(2, 0, 1, 3).reshape(block, HEADS * head_dim).astype(jnp.bfloat16)
    attended = lax.map(one_block, blocked).reshape(TOKENS, HEADS * head_dim)
    group_width = HEADS * head_dim // N_TP
    mixed = jnp.zeros((TOKENS, D), jnp.float32)
    for index in range(N_TP):
        columns = attended[:, index * group_width:(index + 1) * group_width]
        rows_out = w_out[index * group_width:(index + 1) * group_width]
        partial_value = jnp.dot(columns, rows_out, preferred_element_type=jnp.float32).astype(jnp.bfloat16)
        mixed = mixed + lax.optimization_barrier(partial_value).astype(jnp.float32)
    updated = latent.astype(jnp.float32) + gate[0] * rms(mixed, post_gain)
    return updated.astype(jnp.bfloat16)
```

```python
import functools
import math

import jax
import jax.numpy as jnp
from jax import lax
from jax.experimental import pallas as pl
from jax.experimental.pallas import tpu as pltpu
from jax.sharding import PartitionSpec as P

GRID_W = 64
EPS = 1e-06
F32 = jnp.float32
BF16 = jnp.bfloat16
MESH = pl.DeviceIdType.MESH


def kernel(
    sizes,
    latent,
    cond,
    ctx_cond,
    context,
    w_shift,
    w_scale,
    w_gate,
    pre_gain,
    post_gain,
    query_gain,
    key_gain,
    w_query,
    w_key,
    w_value,
    w_out,
    out,
    wq,
    wkv,
    wo,
    lat_all,
    mod_part,
    mod_recv,
    gate_part,
    gate_recv,
    mod_all,
    gate_all,
    xn,
    kv_send,
    cx_send,
    q_send,
    kvb,
    cxb,
    qb,
    m_ref,
    l_ref,
    acc_ref,
    att_send,
    att_recv,
    part_send,
    part_recv,
    w_sem,
    lat_ss,
    lat_rs,
    mp_ss,
    mp_rs,
    gp_ss,
    gp_rs,
    ma_ss,
    ma_rs,
    ga_ss,
    ga_rs,
    kva_ss,
    cxa_ss,
    kvz_ss,
    cxz_ss,
    kv_rs,
    cx_rs,
    q_ss,
    q_rs,
    at_ss,
    at_rs,
    pt_ss,
    pt_rs,
):
    n_sp, n_tp, fan, planes, group, hd, tok, rows, ctx = sizes
    width = w_shift.shape[1]
    depth = latent.shape[1]
    qw = group * hd
    me = lax.axis_index("sp")
    mt = lax.axis_index("tp")
    if fan == 1:
        f, g = 0, me
    else:
        f, g = lax.rem(me, fan), lax.div(me, fan)

    def remote(src, dst, ss, rs, **where):
        return pltpu.make_async_remote_copy(
            src_ref=src, dst_ref=dst, send_sem=ss, recv_sem=rs, device_id=where, device_id_type=MESH
        )

    loads = [pltpu.make_async_copy(w_query, wq, w_sem.at[0])]
    kv_loads = []
    for i in range(fan):
        cols = pl.ds(i * hd, hd)
        kv_loads.append(
            pltpu.make_async_copy(w_key.at[:, cols], wkv.at[i, :, pl.ds(0, hd)], w_sem.at[2 + 2 * i])
        )
        kv_loads.append(
            pltpu.make_async_copy(
                w_value.at[:, cols], wkv.at[i, :, pl.ds(hd, hd)], w_sem.at[3 + 2 * i]
            )
        )
    out_load = pltpu.make_async_copy(w_out, wo, w_sem.at[1])
    for copy in kv_loads + loads + [out_load]:
        copy.start()

    bar = pltpu.get_barrier_semaphore()

    @pl.loop(1, n_sp)
    def _(d):
        pl.semaphore_signal(
            bar, inc=1, device_id={"sp": lax.rem(me + d, n_sp)}, device_id_type=MESH
        )

    for d in range(1, n_tp):
        pl.semaphore_signal(
            bar, inc=1, device_id={"tp": lax.rem(mt + d, n_tp)}, device_id_type=MESH
        )

    def silu(v):
        v = v.astype(F32)
        return v / (1.0 + jnp.exp(-v))

    row_id = lax.broadcasted_iota(jnp.int32, (8, cond.shape[1]), 0)
    conds = jnp.where(
        row_id == 0, silu(cond[...]), jnp.where(row_id == 1, silu(ctx_cond[...]), 0.0)
    ).astype(BF16)
    part_shift = jnp.dot(conds, w_shift[...], preferred_element_type=F32)
    part_scale = jnp.dot(conds, w_scale[...], preferred_element_type=F32)
    part_gate = jnp.dot(conds, w_gate[...], preferred_element_type=F32)
    mod_part[0:2, :] = part_shift[0:2]
    mod_part[2:4, :] = part_scale[0:2]
    gate_part[...] = part_gate[0:1]
    pl.semaphore_wait(bar, n_sp - 1 + n_tp - 1)

    def mod_copy(d, slot):
        peer = lax.rem(me + d, n_sp)
        return remote(mod_part, mod_recv.at[slot], mp_ss.at[d], mp_rs.at[slot], sp=peer)

    def gate_copy(d, slot):
        peer = lax.rem(me + d, n_sp)
        return remote(gate_part, gate_recv.at[slot], gp_ss.at[d], gp_rs.at[slot], sp=peer)

    @pl.loop(1, n_sp)
    def _(d):
        mod_copy(d, me).start()

    def lat_copy(d, slot):
        peer = lax.rem(mt + d, n_tp)
        return remote(latent, lat_all.at[slot], lat_ss.at[d], lat_rs.at[slot], tp=peer)

    for d in range(1, n_tp):
        lat_copy(d, mt).start()

    @pl.loop(1, n_sp)
    def _(d):
        gate_copy(d, me).start()

    mod_recv[me] = mod_part[...]
    gate_recv[me] = gate_part[...]
    lat_all[mt] = latent[...]

    lane = lax.broadcasted_iota(jnp.int32, (tok, hd), 1)
    quarter = hd // 4
    pos = (me * tok + lax.broadcasted_iota(jnp.int32, (tok, hd), 0)).astype(F32)
    row_pos = jnp.floor(pos * (1.0 / GRID_W))
    col_pos = pos - row_pos * GRID_W
    step = (lane & (quarter - 1)).astype(F32)
    freq = jnp.exp(step * (-2.0 * math.log(10000.0) / (hd // 2)))
    angle = jnp.where(lane < hd // 2, row_pos, col_pos) * freq
    low = (lane & quarter) == 0
    cosine = jnp.cos(angle)
    sine = jnp.sin(angle)
    sine = jnp.where(low, -sine, sine)

    def head_rms(v, gain):
        return v * lax.rsqrt(jnp.mean(v * v, axis=-1, keepdims=True) + EPS) * gain

    def rotate(v):
        other = jnp.where(low, pltpu.roll(v, hd - quarter, 1), pltpu.roll(v, quarter, 1))
        return v * cosine + other * sine

    for d in range(1, n_tp):
        lat_copy(d, lax.rem(mt + d, n_tp)).wait_recv()

    def inverse(v):
        return lax.rsqrt(jnp.mean(v * v, axis=-1, keepdims=True) + EPS)

    lat_inv = [inverse(lat_all[t].astype(F32)) for t in range(n_tp)]
    ctx_inv = inverse(context[...].astype(F32))

    @pl.loop(1, n_sp)
    def _(d):
        mod_copy(d, lax.rem(me + d, n_sp)).wait_recv()

    total = lax.fori_loop(
        1, n_sp, lambda i, s: s + mod_recv[i], mod_recv[0]
    )
    mod_all[mt] = total

    def ma_copy(d, slot):
        peer = lax.rem(mt + d, n_tp)
        return remote(mod_all.at[mt], mod_all.at[slot], ma_ss.at[d], ma_rs.at[slot], tp=peer)

    for d in range(1, n_tp):
        ma_copy(d, mt).start()
    for d in range(1, n_tp):
        ma_copy(d, lax.rem(mt + d, n_tp)).wait_recv()

    for t in range(n_tp):
        cols = slice(t * width, (t + 1) * width)
        shift0, shift1 = mod_all[t, 0:1], mod_all[t, 1:2]
        scale0, scale1 = mod_all[t, 2:3], mod_all[t, 3:4]
        gain = pre_gain[:, cols]
        for s in range(n_tp):
            v = lat_all[s, :, cols].astype(F32) * lat_inv[s] * gain
            xn[s * rows : (s + 1) * rows, cols] = (v * (1.0 + scale0) + shift0).astype(BF16)
        v = context[:, cols].astype(F32) * ctx_inv * gain
        xn[tok : tok + ctx, cols] = (v * (1.0 + scale1) + shift1).astype(BF16)

    for copy in kv_loads:
        copy.wait()
    mine = pl.ds(pl.multiple_of(f * tok, tok), tok) if fan > 1 else pl.ds(0, tok)
    mine_c = pl.ds(pl.multiple_of(f * ctx, ctx), ctx) if fan > 1 else pl.ds(0, ctx)

    def block_rows(i):
        if fan == 1:
            return pl.ds(0, tok), pl.ds(0, ctx)
        return (
            pl.ds(pl.multiple_of(i * tok, tok), tok),
            pl.ds(pl.multiple_of(i * ctx, ctx), ctx),
        )

    def chip(plane, i):
        return plane * fan + i

    def project_kv(i):
        both = jnp.dot(xn[...], wkv[i], preferred_element_type=F32)
        k = head_rms(both[:, :hd], key_gain[...])
        v = both[:, hd:].astype(BF16)
        key = rotate(k[:tok]).astype(BF16)
        return key, v[:tok], k[tok:].astype(BF16), v[tok:]

    def kva_copy(i):
        return remote(
            kv_send.at[i], kvb.at[g, :, mine], kva_ss.at[i], kv_rs.at[me], sp=chip(g, i)
        )

    def cxa_copy(i):
        return remote(
            cx_send.at[i], cxb.at[g, :, mine_c], cxa_ss.at[i], cx_rs.at[me], sp=chip(g, i)
        )

    def kvz_copy(way, plane, i):
        r, rc = block_rows(i)
        src = chip(plane, i)
        peer = me + fan if way == 0 else me - fan
        return remote(
            kvb.at[plane, :, r], kvb.at[plane, :, r], kvz_ss.at[way, src], kv_rs.at[src], sp=peer
        )

    def cxz_copy(way, plane, i):
        r, rc = block_rows(i)
        src = chip(plane, i)
        peer = me + fan if way == 0 else me - fan
        return remote(
            cxb.at[plane, :, rc], cxb.at[plane, :, rc], cxz_ss.at[way, src], cx_rs.at[src], sp=peer
        )

    def pass_on(way, plane, i):
        room = g < planes - 1 if way == 0 else g > 0

        @pl.when(room)
        def _():
            kvz_copy(way, plane, i).start()
            cxz_copy(way, plane, i).start()

    def block_wait(plane, i):
        kvz_copy(0, plane, i).wait_recv()
        cxz_copy(0, plane, i).wait_recv()

    key, val, ckey, cval = project_kv(f)
    kvb[g, 0, mine] = key
    kvb[g, 1, mine] = val
    cxb[g, 0, mine_c] = ckey
    cxb[g, 1, mine_c] = cval
    pass_on(0, g, f)
    pass_on(1, g, f)
    for d in range(1, fan):
        i = lax.rem(f + d, fan)
        key, val, ckey, cval = project_kv(i)
        kv_send[i, 0] = key
        kv_send[i, 1] = val
        cx_send[i, 0] = ckey
        cx_send[i, 1] = cval
        kva_copy(i).start()
        cxa_copy(i).start()

    for copy in loads:
        copy.wait()

    def project_q(i):
        if fan == 1:
            w = wq[...]
        else:
            w = wq[:, pl.ds(pl.multiple_of(i * qw, qw), qw)]
        q = jnp.dot(xn[0:tok], w, preferred_element_type=F32)
        return [
            rotate(head_rms(q[:, h * hd : (h + 1) * hd], query_gain[...])).astype(BF16)
            for h in range(group)
        ]

    def q_copy(i, slot):
        return remote(q_send.at[i], qb.at[slot], q_ss.at[i], q_rs.at[slot], sp=chip(g, i))

    for d in range(1, fan):
        i = lax.rem(f + d, fan)
        for h, q in enumerate(project_q(i)):
            q_send[i, h] = q
        q_copy(i, f).start()
        j = lax.rem(f + fan - d, fan)
        block_wait(g, j)
        pass_on(0, g, j)
        pass_on(1, g, j)
    for h, q in enumerate(project_q(f)):
        qb[f, h] = q
    m_ref[...] = jnp.full(m_ref.shape, -1e30, F32)
    l_ref[...] = jnp.zeros(l_ref.shape, F32)
    acc_ref[...] = jnp.zeros(acc_ref.shape, F32)
    for d in range(1, fan):
        q_copy(f, lax.rem(f + d, fan)).wait_recv()

    root = math.sqrt(hd)
    lift = math.log(tok * n_sp / (4.0 * ctx * n_sp)) * root
    factor = math.log2(math.e) / root
    contract = (((1,), (1,)), ((), ()))

    def attend(plane):
        @pl.loop(0, fan)
        def _(i):
            for h in range(group):
                q = qb[i, h]
                s = lax.dot_general(q, kvb[plane, 0], contract, preferred_element_type=F32)
                c = lax.dot_general(q, cxb[plane, 0], contract, preferred_element_type=F32) + lift
                old = m_ref[i, h]
                new = jnp.maximum(
                    jnp.maximum(old, jnp.max(s, axis=-1, keepdims=True)),
                    jnp.max(c, axis=-1, keepdims=True),
                )
                fade = jnp.exp2((old - new) * factor)
                s = jnp.exp2((s - new) * factor)
                c = jnp.exp2((c - new) * factor)
                m_ref[i, h] = new
                l_ref[i, h] = (
                    l_ref[i, h] * fade
                    + jnp.sum(s, axis=-1, keepdims=True)
                    + jnp.sum(c, axis=-1, keepdims=True)
                )
                acc_ref[i, h] = (
                    acc_ref[i, h] * fade
                    + jnp.dot(s.astype(BF16), kvb[plane, 1], preferred_element_type=F32)
                    + jnp.dot(c.astype(BF16), cxb[plane, 1], preferred_element_type=F32)
                )

    attend(g)

    @pl.loop(1, planes)
    def _(t):
        for d in range(fan):
            i = lax.rem(f + fan - d, fan) if fan > 1 else 0

            @pl.when(g - t >= 0)
            def _():
                block_wait(g - t, i)
                pass_on(0, g - t, i)

            @pl.when(g + t < planes)
            def _():
                block_wait(g + t, i)
                pass_on(1, g + t, i)

        @pl.when(g - t >= 0)
        def _():
            attend(g - t)

        @pl.when(g + t < planes)
        def _():
            attend(g + t)

    def at_copy(i, slot):
        return remote(
            att_send.at[i], att_recv.at[slot], at_ss.at[i], at_rs.at[slot], sp=chip(g, i)
        )

    def attended(i):
        return [(acc_ref[i, h] / l_ref[i, h]).astype(BF16) for h in range(group)]

    for d in range(1, fan):
        i = lax.rem(f + d, fan)
        for h, a in enumerate(attended(i)):
            att_send[i, :, h * hd : (h + 1) * hd] = a
        at_copy(i, f).start()
    for h, a in enumerate(attended(f)):
        att_recv[f, :, h * hd : (h + 1) * hd] = a

    @pl.loop(1, n_sp)
    def _(d):
        gate_copy(d, lax.rem(me + d, n_sp)).wait_recv()

    gate_all[mt] = lax.fori_loop(1, n_sp, lambda i, s: s + gate_recv[i], gate_recv[0])

    def ga_copy(d, slot):
        peer = lax.rem(mt + d, n_tp)
        return remote(gate_all.at[mt], gate_all.at[slot], ga_ss.at[d], ga_rs.at[slot], tp=peer)

    for d in range(1, n_tp):
        ga_copy(d, mt).start()
    out_load.wait()
    for d in range(1, fan):
        at_copy(f, lax.rem(f + d, fan)).wait_recv()

    def project_out(t):
        r = pl.ds(pl.multiple_of(t * rows, rows), rows)
        wide = jnp.concatenate([att_recv[i, r] for i in range(fan)], axis=-1)
        return jnp.dot(wide, wo[...], preferred_element_type=F32).astype(BF16)

    def pt_copy(d, t, slot):
        return remote(part_send.at[t], part_recv.at[slot], pt_ss.at[t], pt_rs.at[slot], tp=t)

    for d in range(1, n_tp):
        t = lax.rem(mt + d, n_tp)
        part_send[t] = project_out(t)
        pt_copy(d, t, mt).start()
    part_recv[mt] = project_out(mt)
    for d in range(1, n_tp):
        ga_copy(d, lax.rem(mt + d, n_tp)).wait_recv()
    for d in range(1, n_tp):
        t = lax.rem(mt + d, n_tp)
        pt_copy(d, t, t).wait_recv()
    mixed = part_recv[0].astype(F32)
    for t in range(1, n_tp):
        mixed = mixed + part_recv[t].astype(F32)
    inv = lax.rsqrt(jnp.mean(mixed * mixed, axis=-1, keepdims=True) + EPS)
    for t in range(n_tp):
        cols = slice(t * width, (t + 1) * width)
        out[:, cols] = (
            latent[:, cols].astype(F32)
            + gate_all[t] * (mixed[:, cols] * inv * post_gain[:, cols])
        ).astype(BF16)

    @pl.loop(1, n_sp)
    def _(d):
        mod_copy(d, me).wait_send()
        gate_copy(d, me).wait_send()

    for d in range(1, n_tp):
        lat_copy(d, mt).wait_send()
        ma_copy(d, mt).wait_send()
        ga_copy(d, mt).wait_send()
        t = lax.rem(mt + d, n_tp)
        pt_copy(d, t, mt).wait_send()
    for d in range(1, fan):
        i = lax.rem(f + d, fan)
        kva_copy(i).wait_send()
        cxa_copy(i).wait_send()
        q_copy(i, f).wait_send()
        at_copy(i, f).wait_send()

    @pl.loop(0, planes)
    def _(plane):
        for i in range(fan):

            @pl.when((plane <= g) & (g < planes - 1))
            def _():
                kvz_copy(0, plane, i).wait_send()
                cxz_copy(0, plane, i).wait_send()

            @pl.when((plane >= g) & (g > 0))
            def _():
                kvz_copy(1, plane, i).wait_send()
                cxz_copy(1, plane, i).wait_send()


def body(
    latent,
    condition,
    context_condition,
    context,
    w_shift,
    w_scale,
    w_gate,
    pre_gain,
    post_gain,
    query_gain,
    key_gain,
    w_query,
    w_key,
    w_value,
    w_out,
):
    n_sp = lax.axis_size("sp")
    n_tp = lax.axis_size("tp")
    hd = query_gain.shape[0]
    kv_dev = w_key.shape[1] // hd
    group = w_query.shape[1] // w_key.shape[1]
    fan = kv_dev
    planes = n_sp // fan
    rows, depth = latent.shape
    tok = rows * n_tp
    ctx = context.shape[0]
    width = w_shift.shape[1]
    sizes = (n_sp, n_tp, fan, planes, group, hd, tok, rows, ctx)
    vmem = pl.BlockSpec(memory_space=pltpu.VMEM)
    hbm = pl.BlockSpec(memory_space=pl.ANY)
    dma = pltpu.SemaphoreType.DMA
    scratch = [
        pltpu.VMEM(w_query.shape, BF16),
        pltpu.VMEM((fan, depth, 2 * hd), BF16),
        pltpu.VMEM(w_out.shape, BF16),
        pltpu.VMEM((n_tp, rows, depth), BF16),
        pltpu.VMEM((4, width), F32),
        pltpu.VMEM((n_sp, 4, width), F32),
        pltpu.VMEM((1, width), F32),
        pltpu.VMEM((n_sp, 1, width), F32),
        pltpu.VMEM((n_tp, 4, width), F32),
        pltpu.VMEM((n_tp, 1, width), F32),
        pltpu.VMEM((tok + ctx, depth), BF16),
        pltpu.VMEM((fan, 2, tok, hd), BF16),
        pltpu.VMEM((fan, 2, ctx, hd), BF16),
        pltpu.VMEM((fan, group, tok, hd), BF16),
        pltpu.VMEM((planes, 2, fan * tok, hd), BF16),
        pltpu.VMEM((planes, 2, fan * ctx, hd), BF16),
        pltpu.VMEM((fan, group, tok, hd), BF16),
        pltpu.VMEM((fan, group, tok, 1), F32),
        pltpu.VMEM((fan, group, tok, 1), F32),
        pltpu.VMEM((fan, group, tok, hd), F32),
        pltpu.VMEM((fan, tok, group * hd), BF16),
        pltpu.VMEM((fan, tok, group * hd), BF16),
        pltpu.VMEM((n_tp, rows, depth), BF16),
        pltpu.VMEM((n_tp, rows, depth), BF16),
        dma((2 + 2 * fan,)),
        dma((n_tp,)),
        dma((n_tp,)),
        dma((n_sp,)),
        dma((n_sp,)),
        dma((n_sp,)),
        dma((n_sp,)),
        dma((n_tp,)),
        dma((n_tp,)),
        dma((n_tp,)),
        dma((n_tp,)),
        dma((fan,)),
        dma((fan,)),
        dma((2, n_sp)),
        dma((2, n_sp)),
        dma((n_sp,)),
        dma((n_sp,)),
        dma((fan,)),
        dma((fan,)),
        dma((fan,)),
        dma((fan,)),
        dma((n_tp,)),
        dma((n_tp,)),
    ]
    return pl.pallas_call(
        functools.partial(kernel, sizes),
        out_shape=jax.ShapeDtypeStruct(latent.shape, BF16),
        in_specs=[vmem] * 11 + [hbm] * 4,
        out_specs=vmem,
        scratch_shapes=scratch,
        compiler_params=pltpu.CompilerParams(
            collective_id=0, has_side_effects=True, vmem_limit_bytes=60 * 1024 * 1024
        ),
    )(
        latent,
        condition.reshape(1, -1),
        context_condition.reshape(1, -1),
        context,
        w_shift,
        w_scale,
        w_gate,
        pre_gain.reshape(1, -1),
        post_gain.reshape(1, -1),
        query_gain.reshape(1, -1),
        key_gain.reshape(1, -1),
        w_query,
        w_key,
        w_value,
        w_out,
    )


def solution(mesh):
    placed = (
        P(("sp", "tp"), None),
        P("sp"),
        P("sp"),
        P("sp", None),
        P("sp", "tp"),
        P("sp", "tp"),
        P("sp", "tp"),
        P(),
        P(),
        P(),
        P(),
        P(None, "tp"),
        P(None, "tp"),
        P(None, "tp"),
        P("tp", None),
    )
    return jax.shard_map(
        body, mesh=mesh, in_specs=placed, out_specs=P(("sp", "tp"), None), check_vma=False
    )
```

```python
import functools
import math

import jax
import jax.numpy as jnp
from jax import lax
from jax.experimental import pallas as pl
from jax.experimental.pallas import tpu as pltpu
from jax.sharding import PartitionSpec as P

GRID_W = 64
EPS = 1e-06
F32 = jnp.float32
BF16 = jnp.bfloat16
MESH = pl.DeviceIdType.MESH


def kernel(
    sizes,
    latent,
    cond,
    ctx_cond,
    context,
    w_shift,
    w_scale,
    w_gate,
    pre_gain,
    post_gain,
    query_gain,
    key_gain,
    w_query,
    w_key,
    w_value,
    w_out,
    out,
    wq,
    wkv,
    wo,
    lat_all,
    mod_part,
    mod_recv,
    gate_part,
    gate_recv,
    mod_all,
    gate_all,
    xn,
    kv_send,
    cx_send,
    q_send,
    kvb,
    cxb,
    qb,
    m_ref,
    l_ref,
    acc_ref,
    att_send,
    att_recv,
    part_send,
    part_recv,
    w_sem,
    lat_ss,
    lat_rs,
    mp_ss,
    mp_rs,
    gp_ss,
    gp_rs,
    ma_ss,
    ma_rs,
    ga_ss,
    ga_rs,
    kva_ss,
    cxa_ss,
    kvz_ss,
    cxz_ss,
    kv_rs,
    cx_rs,
    q_ss,
    q_rs,
    at_ss,
    at_rs,
    pt_ss,
    pt_rs,
):
    n_sp, n_tp, fan, planes, group, hd, tok, rows, ctx = sizes
    width = w_shift.shape[1]
    depth = latent.shape[1]
    qw = group * hd
    me = lax.axis_index("sp")
    mt = lax.axis_index("tp")
    if fan == 1:
        f, g = 0, me
    else:
        f, g = lax.rem(me, fan), lax.div(me, fan)

    def remote(src, dst, ss, rs, **where):
        return pltpu.make_async_remote_copy(
            src_ref=src, dst_ref=dst, send_sem=ss, recv_sem=rs, device_id=where, device_id_type=MESH
        )

    loads = [pltpu.make_async_copy(w_query, wq, w_sem.at[0])]
    kv_loads = []
    for i in range(fan):
        cols = pl.ds(i * hd, hd)
        kv_loads.append(
            pltpu.make_async_copy(w_key.at[:, cols], wkv.at[i, :, pl.ds(0, hd)], w_sem.at[2 + 2 * i])
        )
        kv_loads.append(
            pltpu.make_async_copy(
                w_value.at[:, cols], wkv.at[i, :, pl.ds(hd, hd)], w_sem.at[3 + 2 * i]
            )
        )
    out_load = pltpu.make_async_copy(w_out, wo, w_sem.at[1])
    for copy in kv_loads + loads + [out_load]:
        copy.start()

    bar = pltpu.get_barrier_semaphore()

    @pl.loop(1, n_sp)
    def _(d):
        pl.semaphore_signal(
            bar, inc=1, device_id={"sp": lax.rem(me + d, n_sp)}, device_id_type=MESH
        )

    for d in range(1, n_tp):
        pl.semaphore_signal(
            bar, inc=1, device_id={"tp": lax.rem(mt + d, n_tp)}, device_id_type=MESH
        )

    def silu(v):
        v = v.astype(F32)
        return v / (1.0 + jnp.exp(-v))

    row_id = lax.broadcasted_iota(jnp.int32, (8, cond.shape[1]), 0)
    conds = jnp.where(
        row_id == 0, silu(cond[...]), jnp.where(row_id == 1, silu(ctx_cond[...]), 0.0)
    ).astype(BF16)
    part_shift = jnp.dot(conds, w_shift[...], preferred_element_type=F32)
    part_scale = jnp.dot(conds, w_scale[...], preferred_element_type=F32)
    part_gate = jnp.dot(conds, w_gate[...], preferred_element_type=F32)
    mod_part[0:2, :] = part_shift[0:2]
    mod_part[2:4, :] = part_scale[0:2]
    gate_part[...] = part_gate[0:1]
    pl.semaphore_wait(bar, n_sp - 1 + n_tp - 1)

    def mod_copy(d, slot):
        peer = lax.rem(me + d, n_sp)
        return remote(mod_part, mod_recv.at[slot], mp_ss.at[d], mp_rs.at[slot], sp=peer)

    def gate_copy(d, slot):
        peer = lax.rem(me + d, n_sp)
        return remote(gate_part, gate_recv.at[slot], gp_ss.at[d], gp_rs.at[slot], sp=peer)

    @pl.loop(1, n_sp)
    def _(d):
        mod_copy(d, me).start()

    def lat_copy(d, slot):
        peer = lax.rem(mt + d, n_tp)
        return remote(latent, lat_all.at[slot], lat_ss.at[d], lat_rs.at[slot], tp=peer)

    for d in range(1, n_tp):
        lat_copy(d, mt).start()

    @pl.loop(1, n_sp)
    def _(d):
        gate_copy(d, me).start()

    mod_recv[me] = mod_part[...]
    gate_recv[me] = gate_part[...]
    lat_all[mt] = latent[...]

    lane = lax.broadcasted_iota(jnp.int32, (tok, hd), 1)
    quarter = hd // 4
    pos = (me * tok + lax.broadcasted_iota(jnp.int32, (tok, hd), 0)).astype(F32)
    row_pos = jnp.floor(pos * (1.0 / GRID_W))
    col_pos = pos - row_pos * GRID_W
    step = (lane & (quarter - 1)).astype(F32)
    freq = jnp.exp(step * (-2.0 * math.log(10000.0) / (hd // 2)))
    angle = jnp.where(lane < hd // 2, row_pos, col_pos) * freq
    low = (lane & quarter) == 0
    cosine = jnp.cos(angle)
    sine = jnp.sin(angle)
    sine = jnp.where(low, -sine, sine)

    def head_rms(v, gain):
        return v * lax.rsqrt(jnp.mean(v * v, axis=-1, keepdims=True) + EPS) * gain

    def rotate(v):
        other = jnp.where(low, pltpu.roll(v, hd - quarter, 1), pltpu.roll(v, quarter, 1))
        return v * cosine + other * sine

    for d in range(1, n_tp):
        lat_copy(d, lax.rem(mt + d, n_tp)).wait_recv()

    def inverse(v):
        return lax.rsqrt(jnp.mean(v * v, axis=-1, keepdims=True) + EPS)

    lat_inv = [inverse(lat_all[t].astype(F32)) for t in range(n_tp)]
    ctx_inv = inverse(context[...].astype(F32))

    @pl.loop(1, n_sp)
    def _(d):
        mod_copy(d, lax.rem(me + d, n_sp)).wait_recv()

    total = lax.fori_loop(
        1, n_sp, lambda i, s: s + mod_recv[i], mod_recv[0]
    )
    mod_all[mt] = total

    def ma_copy(d, slot):
        peer = lax.rem(mt + d, n_tp)
        return remote(mod_all.at[mt], mod_all.at[slot], ma_ss.at[d], ma_rs.at[slot], tp=peer)

    for d in range(1, n_tp):
        ma_copy(d, mt).start()
    for d in range(1, n_tp):
        ma_copy(d, lax.rem(mt + d, n_tp)).wait_recv()

    for t in range(n_tp):
        cols = slice(t * width, (t + 1) * width)
        shift0, shift1 = mod_all[t, 0:1], mod_all[t, 1:2]
        scale0, scale1 = mod_all[t, 2:3], mod_all[t, 3:4]
        gain = pre_gain[:, cols]
        for s in range(n_tp):
            v = lat_all[s, :, cols].astype(F32) * lat_inv[s] * gain
            xn[s * rows : (s + 1) * rows, cols] = (v * (1.0 + scale0) + shift0).astype(BF16)
        v = context[:, cols].astype(F32) * ctx_inv * gain
        xn[tok : tok + ctx, cols] = (v * (1.0 + scale1) + shift1).astype(BF16)

    for copy in kv_loads:
        copy.wait()
    mine = pl.ds(pl.multiple_of(f * tok, tok), tok) if fan > 1 else pl.ds(0, tok)
    mine_c = pl.ds(pl.multiple_of(f * ctx, ctx), ctx) if fan > 1 else pl.ds(0, ctx)

    def block_rows(i):
        if fan == 1:
            return pl.ds(0, tok), pl.ds(0, ctx)
        return (
            pl.ds(pl.multiple_of(i * tok, tok), tok),
            pl.ds(pl.multiple_of(i * ctx, ctx), ctx),
        )

    def chip(plane, i):
        return plane * fan + i

    def project_kv(i):
        both = jnp.dot(xn[...], wkv[i], preferred_element_type=F32)
        k = head_rms(both[:, :hd], key_gain[...])
        v = both[:, hd:].astype(BF16)
        key = rotate(k[:tok]).astype(BF16)
        return key, v[:tok], k[tok:].astype(BF16), v[tok:]

    def kva_copy(i):
        return remote(
            kv_send.at[i], kvb.at[g, :, mine], kva_ss.at[i], kv_rs.at[me], sp=chip(g, i)
        )

    def cxa_copy(i):
        return remote(
            cx_send.at[i], cxb.at[g, :, mine_c], cxa_ss.at[i], cx_rs.at[me], sp=chip(g, i)
        )

    def kvz_copy(way, plane, i):
        r, rc = block_rows(i)
        src = chip(plane, i)
        peer = me + fan if way == 0 else me - fan
        return remote(
            kvb.at[plane, :, r], kvb.at[plane, :, r], kvz_ss.at[way, src], kv_rs.at[src], sp=peer
        )

    def cxz_copy(way, plane, i):
        r, rc = block_rows(i)
        src = chip(plane, i)
        peer = me + fan if way == 0 else me - fan
        return remote(
            cxb.at[plane, :, rc], cxb.at[plane, :, rc], cxz_ss.at[way, src], cx_rs.at[src], sp=peer
        )

    def pass_on(way, plane, i):
        room = g < planes - 1 if way == 0 else g > 0

        @pl.when(room)
        def _():
            kvz_copy(way, plane, i).start()
            cxz_copy(way, plane, i).start()

    def block_wait(plane, i):
        kvz_copy(0, plane, i).wait_recv()
        cxz_copy(0, plane, i).wait_recv()

    key, val, ckey, cval = project_kv(f)
    kvb[g, 0, mine] = key
    kvb[g, 1, mine] = val
    cxb[g, 0, mine_c] = ckey
    cxb[g, 1, mine_c] = cval
    pass_on(0, g, f)
    pass_on(1, g, f)
    for d in range(1, fan):
        i = lax.rem(f + d, fan)
        key, val, ckey, cval = project_kv(i)
        kv_send[i, 0] = key
        kv_send[i, 1] = val
        cx_send[i, 0] = ckey
        cx_send[i, 1] = cval
        kva_copy(i).start()
        cxa_copy(i).start()

    for copy in loads:
        copy.wait()

    def project_q(i):
        if fan == 1:
            w = wq[...]
        else:
            w = wq[:, pl.ds(pl.multiple_of(i * qw, qw), qw)]
        q = jnp.dot(xn[0:tok], w, preferred_element_type=F32)
        return [
            rotate(head_rms(q[:, h * hd : (h + 1) * hd], query_gain[...])).astype(BF16)
            for h in range(group)
        ]

    def q_copy(i, slot):
        return remote(q_send.at[i], qb.at[slot], q_ss.at[i], q_rs.at[slot], sp=chip(g, i))

    for d in range(1, fan):
        i = lax.rem(f + d, fan)
        for h, q in enumerate(project_q(i)):
            q_send[i, h] = q
        q_copy(i, f).start()
        j = lax.rem(f + fan - d, fan)
        block_wait(g, j)
        pass_on(0, g, j)
        pass_on(1, g, j)
    for h, q in enumerate(project_q(f)):
        qb[f, h] = q
    m_ref[...] = jnp.full(m_ref.shape, -1e30, F32)
    l_ref[...] = jnp.zeros(l_ref.shape, F32)
    acc_ref[...] = jnp.zeros(acc_ref.shape, F32)
    root = math.sqrt(hd)
    lift = math.log(tok * n_sp / (4.0 * ctx * n_sp)) * root
    factor = math.log2(math.e) / root
    contract = (((1,), (1,)), ((), ()))

    def absorb(i, key, value, ckey, cvalue):
        for h in range(group):
            q = qb[i, h]
            s = lax.dot_general(q, key, contract, preferred_element_type=F32)
            c = lax.dot_general(q, ckey, contract, preferred_element_type=F32) + lift
            old = m_ref[i, h]
            new = jnp.maximum(
                jnp.maximum(old, jnp.max(s, axis=-1, keepdims=True)),
                jnp.max(c, axis=-1, keepdims=True),
            )
            fade = jnp.exp2((old - new) * factor)
            s = jnp.exp2((s - new) * factor)
            c = jnp.exp2((c - new) * factor)
            m_ref[i, h] = new
            l_ref[i, h] = (
                l_ref[i, h] * fade
                + jnp.sum(s, axis=-1, keepdims=True)
                + jnp.sum(c, axis=-1, keepdims=True)
            )
            acc_ref[i, h] = (
                acc_ref[i, h] * fade
                + jnp.dot(s.astype(BF16), value, preferred_element_type=F32)
                + jnp.dot(c.astype(BF16), cvalue, preferred_element_type=F32)
            )

    def before(n):
        return lax.rem(f + fan - n, fan) if fan > 1 else 0

    def attend(plane, hook):
        @pl.loop(0, fan)
        def _(n):
            hook(n)
            absorb(before(n), kvb[plane, 0], kvb[plane, 1], cxb[plane, 0], cxb[plane, 1])

    def at_copy(i, slot):
        return remote(
            att_send.at[i], att_recv.at[slot], at_ss.at[i], at_rs.at[slot], sp=chip(g, i)
        )

    def attended(i):
        return [(acc_ref[i, h] / l_ref[i, h]).astype(BF16) for h in range(group)]

    def give(n, i):
        @pl.when(n < fan - 1)
        def _():
            for h, a in enumerate(attended(i)):
                att_send[i, :, h * hd : (h + 1) * hd] = a
            at_copy(i, f).start()

        @pl.when(n == fan - 1)
        def _():
            for h, a in enumerate(attended(f)):
                att_recv[f, :, h * hd : (h + 1) * hd] = a

    def after(n):
        return lax.rem(f + 1 + n, fan) if fan > 1 else 0

    top, bottom = g == planes - 1, g == 0
    edge = top | bottom

    def arrive(t, n):
        i = before(n)

        @pl.when((g - t >= 0) & (g < planes - 1))
        def _():
            block_wait(g - t, i)
            pass_on(0, g - t, i)

        @pl.when((g + t < planes) & (g > 0))
        def _():
            block_wait(g + t, i)
            pass_on(1, g + t, i)

    def first_hook(n):
        if fan > 1:

            @pl.when(n > 0)
            def _():
                q_copy(f, before(n)).wait_recv()

        arrive(1, n)

    attend(g, first_hook)

    @pl.loop(1, planes - 1)
    def _(t):
        for n in range(fan):

            @pl.when(top)
            def _():
                block_wait(g - t, before(n))

            @pl.when(bottom)
            def _():
                block_wait(g + t, before(n))

        @pl.when(g - t >= 0)
        def _():
            attend(g - t, lambda n: arrive(t + 1, n))

        @pl.when((g + t < planes) & (g - t < 0))
        def _():
            attend(g + t, lambda n: arrive(t + 1, n))

        @pl.when((g + t < planes) & (g - t >= 0))
        def _():
            attend(g + t, lambda n: None)

    @pl.when(edge)
    def _():
        far = jnp.where(bottom, planes - 1, 0)

        @pl.loop(0, fan)
        def _(d):
            j = before(d)
            r, rc = block_rows(j)
            block_wait(far, j)

            @pl.loop(0, fan)
            def _(n):
                i = after(n)
                absorb(i, kvb[far, 0, r], kvb[far, 1, r], cxb[far, 0, rc], cxb[far, 1, rc])

                @pl.when(d == fan - 1)
                def _():
                    give(n, i)

    @pl.when(jnp.logical_not(edge))
    def _():
        @pl.loop(0, fan)
        def _(n):
            give(n, after(n))

    @pl.loop(1, n_sp)
    def _(d):
        gate_copy(d, lax.rem(me + d, n_sp)).wait_recv()

    gate_all[mt] = lax.fori_loop(1, n_sp, lambda i, s: s + gate_recv[i], gate_recv[0])

    def ga_copy(d, slot):
        peer = lax.rem(mt + d, n_tp)
        return remote(gate_all.at[mt], gate_all.at[slot], ga_ss.at[d], ga_rs.at[slot], tp=peer)

    for d in range(1, n_tp):
        ga_copy(d, mt).start()
    out_load.wait()
    for d in range(1, fan):
        at_copy(f, lax.rem(f + d, fan)).wait_recv()

    def project_out(t):
        r = pl.ds(pl.multiple_of(t * rows, rows), rows)
        wide = jnp.concatenate([att_recv[i, r] for i in range(fan)], axis=-1)
        return jnp.dot(wide, wo[...], preferred_element_type=F32).astype(BF16)

    def pt_copy(d, t, slot):
        return remote(part_send.at[t], part_recv.at[slot], pt_ss.at[t], pt_rs.at[slot], tp=t)

    for d in range(1, n_tp):
        t = lax.rem(mt + d, n_tp)
        part_send[t] = project_out(t)
        pt_copy(d, t, mt).start()
    part_recv[mt] = project_out(mt)
    for d in range(1, n_tp):
        ga_copy(d, lax.rem(mt + d, n_tp)).wait_recv()
    for d in range(1, n_tp):
        t = lax.rem(mt + d, n_tp)
        pt_copy(d, t, t).wait_recv()
    mixed = part_recv[0].astype(F32)
    for t in range(1, n_tp):
        mixed = mixed + part_recv[t].astype(F32)
    inv = lax.rsqrt(jnp.mean(mixed * mixed, axis=-1, keepdims=True) + EPS)
    for t in range(n_tp):
        cols = slice(t * width, (t + 1) * width)
        out[:, cols] = (
            latent[:, cols].astype(F32)
            + gate_all[t] * (mixed[:, cols] * inv * post_gain[:, cols])
        ).astype(BF16)

    @pl.loop(1, n_sp)
    def _(d):
        mod_copy(d, me).wait_send()
        gate_copy(d, me).wait_send()

    for d in range(1, n_tp):
        lat_copy(d, mt).wait_send()
        ma_copy(d, mt).wait_send()
        ga_copy(d, mt).wait_send()
        t = lax.rem(mt + d, n_tp)
        pt_copy(d, t, mt).wait_send()
    for d in range(1, fan):
        i = lax.rem(f + d, fan)
        kva_copy(i).wait_send()
        cxa_copy(i).wait_send()
        q_copy(i, f).wait_send()
        at_copy(i, f).wait_send()

    @pl.loop(0, planes)
    def _(plane):
        for i in range(fan):

            @pl.when((plane <= g) & (g < planes - 1))
            def _():
                kvz_copy(0, plane, i).wait_send()
                cxz_copy(0, plane, i).wait_send()

            @pl.when((plane >= g) & (g > 0))
            def _():
                kvz_copy(1, plane, i).wait_send()
                cxz_copy(1, plane, i).wait_send()


def body(
    latent,
    condition,
    context_condition,
    context,
    w_shift,
    w_scale,
    w_gate,
    pre_gain,
    post_gain,
    query_gain,
    key_gain,
    w_query,
    w_key,
    w_value,
    w_out,
):
    n_sp = lax.axis_size("sp")
    n_tp = lax.axis_size("tp")
    hd = query_gain.shape[0]
    kv_dev = w_key.shape[1] // hd
    group = w_query.shape[1] // w_key.shape[1]
    fan = kv_dev
    planes = n_sp // fan
    rows, depth = latent.shape
    tok = rows * n_tp
    ctx = context.shape[0]
    width = w_shift.shape[1]
    sizes = (n_sp, n_tp, fan, planes, group, hd, tok, rows, ctx)
    vmem = pl.BlockSpec(memory_space=pltpu.VMEM)
    hbm = pl.BlockSpec(memory_space=pl.ANY)
    dma = pltpu.SemaphoreType.DMA
    scratch = [
        pltpu.VMEM(w_query.shape, BF16),
        pltpu.VMEM((fan, depth, 2 * hd), BF16),
        pltpu.VMEM(w_out.shape, BF16),
        pltpu.VMEM((n_tp, rows, depth), BF16),
        pltpu.VMEM((4, width), F32),
        pltpu.VMEM((n_sp, 4, width), F32),
        pltpu.VMEM((1, width), F32),
        pltpu.VMEM((n_sp, 1, width), F32),
        pltpu.VMEM((n_tp, 4, width), F32),
        pltpu.VMEM((n_tp, 1, width), F32),
        pltpu.VMEM((tok + ctx, depth), BF16),
        pltpu.VMEM((fan, 2, tok, hd), BF16),
        pltpu.VMEM((fan, 2, ctx, hd), BF16),
        pltpu.VMEM((fan, group, tok, hd), BF16),
        pltpu.VMEM((planes, 2, fan * tok, hd), BF16),
        pltpu.VMEM((planes, 2, fan * ctx, hd), BF16),
        pltpu.VMEM((fan, group, tok, hd), BF16),
        pltpu.VMEM((fan, group, tok, 1), F32),
        pltpu.VMEM((fan, group, tok, 1), F32),
        pltpu.VMEM((fan, group, tok, hd), F32),
        pltpu.VMEM((fan, tok, group * hd), BF16),
        pltpu.VMEM((fan, tok, group * hd), BF16),
        pltpu.VMEM((n_tp, rows, depth), BF16),
        pltpu.VMEM((n_tp, rows, depth), BF16),
        dma((2 + 2 * fan,)),
        dma((n_tp,)),
        dma((n_tp,)),
        dma((n_sp,)),
        dma((n_sp,)),
        dma((n_sp,)),
        dma((n_sp,)),
        dma((n_tp,)),
        dma((n_tp,)),
        dma((n_tp,)),
        dma((n_tp,)),
        dma((fan,)),
        dma((fan,)),
        dma((2, n_sp)),
        dma((2, n_sp)),
        dma((n_sp,)),
        dma((n_sp,)),
        dma((fan,)),
        dma((fan,)),
        dma((fan,)),
        dma((fan,)),
        dma((n_tp,)),
        dma((n_tp,)),
    ]
    return pl.pallas_call(
        functools.partial(kernel, sizes),
        out_shape=jax.ShapeDtypeStruct(latent.shape, BF16),
        in_specs=[vmem] * 11 + [hbm] * 4,
        out_specs=vmem,
        scratch_shapes=scratch,
        compiler_params=pltpu.CompilerParams(
            collective_id=0, has_side_effects=True, vmem_limit_bytes=60 * 1024 * 1024
        ),
    )(
        latent,
        condition.reshape(1, -1),
        context_condition.reshape(1, -1),
        context,
        w_shift,
        w_scale,
        w_gate,
        pre_gain.reshape(1, -1),
        post_gain.reshape(1, -1),
        query_gain.reshape(1, -1),
        key_gain.reshape(1, -1),
        w_query,
        w_key,
        w_value,
        w_out,
    )


def solution(mesh):
    placed = (
        P(("sp", "tp"), None),
        P("sp"),
        P("sp"),
        P("sp", None),
        P("sp", "tp"),
        P("sp", "tp"),
        P("sp", "tp"),
        P(),
        P(),
        P(),
        P(),
        P(None, "tp"),
        P(None, "tp"),
        P(None, "tp"),
        P("tp", None),
    )
    return jax.shard_map(
        body, mesh=mesh, in_specs=placed, out_specs=P(("sp", "tp"), None), check_vma=False
    )
```

```python
import functools
import math

import jax
import jax.numpy as jnp
from jax import lax
from jax.experimental import pallas as pl
from jax.experimental.pallas import tpu as pltpu
from jax.sharding import PartitionSpec as P

GRID_W = 64
EPS = 1e-06
F32 = jnp.float32
BF16 = jnp.bfloat16
MESH = pl.DeviceIdType.MESH


def kernel(
    sizes,
    latent,
    cond,
    ctx_cond,
    context,
    w_shift,
    w_scale,
    w_gate,
    pre_gain,
    post_gain,
    query_gain,
    key_gain,
    w_query,
    w_key,
    w_value,
    w_out,
    out,
    wq,
    wkv,
    wo,
    lat_all,
    mod_part,
    mod_recv,
    gate_part,
    gate_recv,
    mod_all,
    gate_all,
    xn,
    kv_send,
    cx_send,
    q_send,
    kvb,
    cxb,
    qb,
    m_ref,
    l_ref,
    acc_ref,
    att_send,
    att_recv,
    part_send,
    part_recv,
    w_sem,
    lat_ss,
    lat_rs,
    mp_ss,
    mp_rs,
    gp_ss,
    gp_rs,
    ma_ss,
    ma_rs,
    ga_ss,
    ga_rs,
    kva_ss,
    cxa_ss,
    kvz_ss,
    cxz_ss,
    kv_rs,
    cx_rs,
    q_ss,
    q_rs,
    at_ss,
    at_rs,
    pt_ss,
    pt_rs,
):
    n_sp, n_tp, fan, planes, group, hd, tok, rows, ctx = sizes
    width = w_shift.shape[1]
    depth = latent.shape[1]
    qw = group * hd
    me = lax.axis_index("sp")
    mt = lax.axis_index("tp")
    if fan == 1:
        f, g = 0, me
    else:
        f, g = lax.rem(me, fan), lax.div(me, fan)

    def remote(src, dst, ss, rs, **where):
        return pltpu.make_async_remote_copy(
            src_ref=src, dst_ref=dst, send_sem=ss, recv_sem=rs, device_id=where, device_id_type=MESH
        )

    loads = [pltpu.make_async_copy(w_query, wq, w_sem.at[0])]
    kv_loads = []
    for i in range(fan):
        cols = pl.ds(i * hd, hd)
        kv_loads.append(
            pltpu.make_async_copy(w_key.at[:, cols], wkv.at[i, :, pl.ds(0, hd)], w_sem.at[2 + 2 * i])
        )
        kv_loads.append(
            pltpu.make_async_copy(
                w_value.at[:, cols], wkv.at[i, :, pl.ds(hd, hd)], w_sem.at[3 + 2 * i]
            )
        )
    out_load = pltpu.make_async_copy(w_out, wo, w_sem.at[1])
    for copy in kv_loads:
        copy.start()

    bar = pltpu.get_barrier_semaphore()

    @pl.loop(1, n_sp)
    def _(d):
        pl.semaphore_signal(
            bar, inc=1, device_id={"sp": lax.rem(me + d, n_sp)}, device_id_type=MESH
        )

    for d in range(1, n_tp):
        pl.semaphore_signal(
            bar, inc=1, device_id={"tp": lax.rem(mt + d, n_tp)}, device_id_type=MESH
        )

    def silu(v):
        v = v.astype(F32)
        return v / (1.0 + jnp.exp(-v))

    row_id = lax.broadcasted_iota(jnp.int32, (8, cond.shape[1]), 0)
    conds = jnp.where(
        row_id == 0, silu(cond[...]), jnp.where(row_id == 1, silu(ctx_cond[...]), 0.0)
    ).astype(BF16)
    part_shift = jnp.dot(conds, w_shift[...], preferred_element_type=F32)
    part_scale = jnp.dot(conds, w_scale[...], preferred_element_type=F32)
    part_gate = jnp.dot(conds, w_gate[...], preferred_element_type=F32)
    mod_part[0:2, :] = part_shift[0:2]
    mod_part[2:4, :] = part_scale[0:2]
    gate_part[...] = part_gate[0:1]
    pl.semaphore_wait(bar, n_sp - 1 + n_tp - 1)

    def mod_copy(d, slot):
        peer = lax.rem(me + d, n_sp)
        return remote(mod_part, mod_recv.at[slot], mp_ss.at[d], mp_rs.at[slot], sp=peer)

    def gate_copy(d, slot):
        peer = lax.rem(me + d, n_sp)
        return remote(gate_part, gate_recv.at[slot], gp_ss.at[d], gp_rs.at[slot], sp=peer)

    @pl.loop(1, n_sp)
    def _(d):
        mod_copy(d, me).start()

    def lat_copy(d, slot):
        peer = lax.rem(mt + d, n_tp)
        return remote(latent, lat_all.at[slot], lat_ss.at[d], lat_rs.at[slot], tp=peer)

    for d in range(1, n_tp):
        lat_copy(d, mt).start()

    for copy in loads + [out_load]:
        copy.start()

    mod_recv[me] = mod_part[...]
    gate_recv[me] = gate_part[...]
    lat_all[mt] = latent[...]

    lane = lax.broadcasted_iota(jnp.int32, (tok, hd), 1)
    quarter = hd // 4
    pos = (me * tok + lax.broadcasted_iota(jnp.int32, (tok, hd), 0)).astype(F32)
    row_pos = jnp.floor(pos * (1.0 / GRID_W))
    col_pos = pos - row_pos * GRID_W
    step = (lane & (quarter - 1)).astype(F32)
    freq = jnp.exp(step * (-2.0 * math.log(10000.0) / (hd // 2)))
    angle = jnp.where(lane < hd // 2, row_pos, col_pos) * freq
    low = (lane & quarter) == 0
    cosine = jnp.cos(angle)
    sine = jnp.sin(angle)
    sine = jnp.where(low, -sine, sine)

    def head_rms(v, gain):
        return v * lax.rsqrt(jnp.mean(v * v, axis=-1, keepdims=True) + EPS) * gain

    def rotate(v):
        other = jnp.where(low, pltpu.roll(v, hd - quarter, 1), pltpu.roll(v, quarter, 1))
        return v * cosine + other * sine

    for d in range(1, n_tp):
        lat_copy(d, lax.rem(mt + d, n_tp)).wait_recv()

    def inverse(v):
        return lax.rsqrt(jnp.mean(v * v, axis=-1, keepdims=True) + EPS)

    lat_inv = [inverse(lat_all[t].astype(F32)) for t in range(n_tp)]
    ctx_inv = inverse(context[...].astype(F32))

    @pl.loop(1, n_sp)
    def _(d):
        mod_copy(d, lax.rem(me + d, n_sp)).wait_recv()

    total = lax.fori_loop(
        1, n_sp, lambda i, s: s + mod_recv[i], mod_recv[0]
    )
    mod_all[mt] = total

    def ma_copy(d, slot):
        peer = lax.rem(mt + d, n_tp)
        return remote(mod_all.at[mt], mod_all.at[slot], ma_ss.at[d], ma_rs.at[slot], tp=peer)

    for d in range(1, n_tp):
        ma_copy(d, mt).start()
    for d in range(1, n_tp):
        ma_copy(d, lax.rem(mt + d, n_tp)).wait_recv()

    for t in range(n_tp):
        cols = slice(t * width, (t + 1) * width)
        shift0, shift1 = mod_all[t, 0:1], mod_all[t, 1:2]
        scale0, scale1 = mod_all[t, 2:3], mod_all[t, 3:4]
        gain = pre_gain[:, cols]
        for s in range(n_tp):
            v = lat_all[s, :, cols].astype(F32) * lat_inv[s] * gain
            xn[s * rows : (s + 1) * rows, cols] = (v * (1.0 + scale0) + shift0).astype(BF16)
        v = context[:, cols].astype(F32) * ctx_inv * gain
        xn[tok : tok + ctx, cols] = (v * (1.0 + scale1) + shift1).astype(BF16)

    for copy in kv_loads:
        copy.wait()
    mine = pl.ds(pl.multiple_of(f * tok, tok), tok) if fan > 1 else pl.ds(0, tok)
    mine_c = pl.ds(pl.multiple_of(f * ctx, ctx), ctx) if fan > 1 else pl.ds(0, ctx)

    def block_rows(i):
        if fan == 1:
            return pl.ds(0, tok), pl.ds(0, ctx)
        return (
            pl.ds(pl.multiple_of(i * tok, tok), tok),
            pl.ds(pl.multiple_of(i * ctx, ctx), ctx),
        )

    def chip(plane, i):
        return plane * fan + i

    def project_kv(i):
        both = jnp.dot(xn[...], wkv[i], preferred_element_type=F32)
        k = head_rms(both[:, :hd], key_gain[...])
        v = both[:, hd:].astype(BF16)
        key = rotate(k[:tok]).astype(BF16)
        return key, v[:tok], k[tok:].astype(BF16), v[tok:]

    def kva_copy(i):
        return remote(
            kv_send.at[i], kvb.at[g, :, mine], kva_ss.at[i], kv_rs.at[me], sp=chip(g, i)
        )

    def cxa_copy(i):
        return remote(
            cx_send.at[i], cxb.at[g, :, mine_c], cxa_ss.at[i], cx_rs.at[me], sp=chip(g, i)
        )

    def kvz_copy(way, plane, i):
        r, rc = block_rows(i)
        src = chip(plane, i)
        peer = me + fan if way == 0 else me - fan
        return remote(
            kvb.at[plane, :, r], kvb.at[plane, :, r], kvz_ss.at[way, src], kv_rs.at[src], sp=peer
        )

    def cxz_copy(way, plane, i):
        r, rc = block_rows(i)
        src = chip(plane, i)
        peer = me + fan if way == 0 else me - fan
        return remote(
            cxb.at[plane, :, rc], cxb.at[plane, :, rc], cxz_ss.at[way, src], cx_rs.at[src], sp=peer
        )

    def pass_on(way, plane, i):
        room = g < planes - 1 if way == 0 else g > 0

        @pl.when(room)
        def _():
            kvz_copy(way, plane, i).start()
            cxz_copy(way, plane, i).start()

    def block_wait(plane, i):
        kvz_copy(0, plane, i).wait_recv()
        cxz_copy(0, plane, i).wait_recv()

    key, val, ckey, cval = project_kv(f)
    kvb[g, 0, mine] = key
    kvb[g, 1, mine] = val
    cxb[g, 0, mine_c] = ckey
    cxb[g, 1, mine_c] = cval
    pass_on(0, g, f)
    pass_on(1, g, f)
    for d in range(1, fan):
        i = lax.rem(f + d, fan)
        key, val, ckey, cval = project_kv(i)
        kv_send[i, 0] = key
        kv_send[i, 1] = val
        cx_send[i, 0] = ckey
        cx_send[i, 1] = cval
        kva_copy(i).start()
        cxa_copy(i).start()

    for copy in loads:
        copy.wait()

    def project_q(i):
        if fan == 1:
            w = wq[...]
        else:
            w = wq[:, pl.ds(pl.multiple_of(i * qw, qw), qw)]
        q = jnp.dot(xn[0:tok], w, preferred_element_type=F32)
        return [
            rotate(head_rms(q[:, h * hd : (h + 1) * hd], query_gain[...])).astype(BF16)
            for h in range(group)
        ]

    def q_copy(i, slot):
        return remote(q_send.at[i], qb.at[slot], q_ss.at[i], q_rs.at[slot], sp=chip(g, i))

    for d in range(1, fan):
        i = lax.rem(f + d, fan)
        for h, q in enumerate(project_q(i)):
            q_send[i, h] = q
        q_copy(i, f).start()
        j = lax.rem(f + fan - d, fan)
        block_wait(g, j)
        pass_on(0, g, j)
        pass_on(1, g, j)
    for h, q in enumerate(project_q(f)):
        qb[f, h] = q
    @pl.loop(1, n_sp)
    def _(d):
        gate_copy(d, me).start()

    m_ref[...] = jnp.full(m_ref.shape, -1e30, F32)
    l_ref[...] = jnp.zeros(l_ref.shape, F32)
    acc_ref[...] = jnp.zeros(acc_ref.shape, F32)
    root = math.sqrt(hd)
    lift = math.log(tok * n_sp / (4.0 * ctx * n_sp)) * root
    factor = math.log2(math.e) / root
    contract = (((1,), (1,)), ((), ()))

    def absorb(i, key, value, ckey, cvalue):
        for h in range(group):
            q = qb[i, h]
            s = lax.dot_general(q, key, contract, preferred_element_type=F32)
            c = lax.dot_general(q, ckey, contract, preferred_element_type=F32) + lift
            old = m_ref[i, h]
            new = jnp.maximum(
                jnp.maximum(old, jnp.max(s, axis=-1, keepdims=True)),
                jnp.max(c, axis=-1, keepdims=True),
            )
            fade = jnp.exp2((old - new) * factor)
            s = jnp.exp2((s - new) * factor)
            c = jnp.exp2((c - new) * factor)
            m_ref[i, h] = new
            l_ref[i, h] = (
                l_ref[i, h] * fade
                + jnp.sum(s, axis=-1, keepdims=True)
                + jnp.sum(c, axis=-1, keepdims=True)
            )
            acc_ref[i, h] = (
                acc_ref[i, h] * fade
                + jnp.dot(s.astype(BF16), value, preferred_element_type=F32)
                + jnp.dot(c.astype(BF16), cvalue, preferred_element_type=F32)
            )

    def before(n):
        return lax.rem(f + fan - n, fan) if fan > 1 else 0

    def attend(plane, hook):
        @pl.loop(0, fan)
        def _(n):
            hook(n)
            absorb(before(n), kvb[plane, 0], kvb[plane, 1], cxb[plane, 0], cxb[plane, 1])

    def at_copy(i, slot):
        return remote(
            att_send.at[i], att_recv.at[slot], at_ss.at[i], at_rs.at[slot], sp=chip(g, i)
        )

    def attended(i):
        return [(acc_ref[i, h] / l_ref[i, h]).astype(BF16) for h in range(group)]

    def give(n, i):
        @pl.when(n < fan - 1)
        def _():
            for h, a in enumerate(attended(i)):
                att_send[i, :, h * hd : (h + 1) * hd] = a
            at_copy(i, f).start()

        @pl.when(n == fan - 1)
        def _():
            for h, a in enumerate(attended(f)):
                att_recv[f, :, h * hd : (h + 1) * hd] = a

    def after(n):
        return lax.rem(f + 1 + n, fan) if fan > 1 else 0

    top, bottom = g == planes - 1, g == 0
    edge = top | bottom

    def arrive(t, n):
        i = before(n)

        @pl.when((g - t >= 0) & (g < planes - 1))
        def _():
            block_wait(g - t, i)
            pass_on(0, g - t, i)

        @pl.when((g + t < planes) & (g > 0))
        def _():
            block_wait(g + t, i)
            pass_on(1, g + t, i)

    def first_hook(n):
        if fan > 1:

            @pl.when(n > 0)
            def _():
                q_copy(f, before(n)).wait_recv()

        arrive(1, n)

    attend(g, first_hook)

    @pl.loop(1, planes - 1)
    def _(t):
        for n in range(fan):

            @pl.when(top)
            def _():
                block_wait(g - t, before(n))

            @pl.when(bottom)
            def _():
                block_wait(g + t, before(n))

        @pl.when(g - t >= 0)
        def _():
            attend(g - t, lambda n: arrive(t + 1, n))

        @pl.when((g + t < planes) & (g - t < 0))
        def _():
            attend(g + t, lambda n: arrive(t + 1, n))

        @pl.when((g + t < planes) & (g - t >= 0))
        def _():
            attend(g + t, lambda n: None)

    @pl.when(edge)
    def _():
        far = jnp.where(bottom, planes - 1, 0)

        @pl.loop(0, fan)
        def _(d):
            j = before(d)
            r, rc = block_rows(j)
            block_wait(far, j)

            @pl.loop(0, fan)
            def _(n):
                i = after(n)
                absorb(i, kvb[far, 0, r], kvb[far, 1, r], cxb[far, 0, rc], cxb[far, 1, rc])

                @pl.when(d == fan - 1)
                def _():
                    give(n, i)

    @pl.when(jnp.logical_not(edge))
    def _():
        @pl.loop(0, fan)
        def _(n):
            give(n, after(n))

    @pl.loop(1, n_sp)
    def _(d):
        gate_copy(d, lax.rem(me + d, n_sp)).wait_recv()

    gate_all[mt] = lax.fori_loop(1, n_sp, lambda i, s: s + gate_recv[i], gate_recv[0])

    def ga_copy(d, slot):
        peer = lax.rem(mt + d, n_tp)
        return remote(gate_all.at[mt], gate_all.at[slot], ga_ss.at[d], ga_rs.at[slot], tp=peer)

    for d in range(1, n_tp):
        ga_copy(d, mt).start()
    out_load.wait()
    for d in range(1, fan):
        at_copy(f, lax.rem(f + d, fan)).wait_recv()

    def project_out(t):
        r = pl.ds(pl.multiple_of(t * rows, rows), rows)
        wide = jnp.concatenate([att_recv[i, r] for i in range(fan)], axis=-1)
        return jnp.dot(wide, wo[...], preferred_element_type=F32).astype(BF16)

    def pt_copy(d, t, slot):
        return remote(part_send.at[t], part_recv.at[slot], pt_ss.at[t], pt_rs.at[slot], tp=t)

    for d in range(1, n_tp):
        t = lax.rem(mt + d, n_tp)
        part_send[t] = project_out(t)
        pt_copy(d, t, mt).start()
    part_recv[mt] = project_out(mt)
    for d in range(1, n_tp):
        ga_copy(d, lax.rem(mt + d, n_tp)).wait_recv()
    for d in range(1, n_tp):
        t = lax.rem(mt + d, n_tp)
        pt_copy(d, t, t).wait_recv()
    mixed = part_recv[0].astype(F32)
    for t in range(1, n_tp):
        mixed = mixed + part_recv[t].astype(F32)
    inv = lax.rsqrt(jnp.mean(mixed * mixed, axis=-1, keepdims=True) + EPS)
    for t in range(n_tp):
        cols = slice(t * width, (t + 1) * width)
        out[:, cols] = (
            latent[:, cols].astype(F32)
            + gate_all[t] * (mixed[:, cols] * inv * post_gain[:, cols])
        ).astype(BF16)

    @pl.loop(1, n_sp)
    def _(d):
        mod_copy(d, me).wait_send()
        gate_copy(d, me).wait_send()

    for d in range(1, n_tp):
        lat_copy(d, mt).wait_send()
        ma_copy(d, mt).wait_send()
        ga_copy(d, mt).wait_send()
        t = lax.rem(mt + d, n_tp)
        pt_copy(d, t, mt).wait_send()
    for d in range(1, fan):
        i = lax.rem(f + d, fan)
        kva_copy(i).wait_send()
        cxa_copy(i).wait_send()
        q_copy(i, f).wait_send()
        at_copy(i, f).wait_send()

    @pl.loop(0, planes)
    def _(plane):
        for i in range(fan):

            @pl.when((plane <= g) & (g < planes - 1))
            def _():
                kvz_copy(0, plane, i).wait_send()
                cxz_copy(0, plane, i).wait_send()

            @pl.when((plane >= g) & (g > 0))
            def _():
                kvz_copy(1, plane, i).wait_send()
                cxz_copy(1, plane, i).wait_send()


def body(
    latent,
    condition,
    context_condition,
    context,
    w_shift,
    w_scale,
    w_gate,
    pre_gain,
    post_gain,
    query_gain,
    key_gain,
    w_query,
    w_key,
    w_value,
    w_out,
):
    n_sp = lax.axis_size("sp")
    n_tp = lax.axis_size("tp")
    hd = query_gain.shape[0]
    kv_dev = w_key.shape[1] // hd
    group = w_query.shape[1] // w_key.shape[1]
    fan = kv_dev
    planes = n_sp // fan
    rows, depth = latent.shape
    tok = rows * n_tp
    ctx = context.shape[0]
    width = w_shift.shape[1]
    sizes = (n_sp, n_tp, fan, planes, group, hd, tok, rows, ctx)
    vmem = pl.BlockSpec(memory_space=pltpu.VMEM)
    hbm = pl.BlockSpec(memory_space=pl.ANY)
    dma = pltpu.SemaphoreType.DMA
    scratch = [
        pltpu.VMEM(w_query.shape, BF16),
        pltpu.VMEM((fan, depth, 2 * hd), BF16),
        pltpu.VMEM(w_out.shape, BF16),
        pltpu.VMEM((n_tp, rows, depth), BF16),
        pltpu.VMEM((4, width), F32),
        pltpu.VMEM((n_sp, 4, width), F32),
        pltpu.VMEM((1, width), F32),
        pltpu.VMEM((n_sp, 1, width), F32),
        pltpu.VMEM((n_tp, 4, width), F32),
        pltpu.VMEM((n_tp, 1, width), F32),
        pltpu.VMEM((tok + ctx, depth), BF16),
        pltpu.VMEM((fan, 2, tok, hd), BF16),
        pltpu.VMEM((fan, 2, ctx, hd), BF16),
        pltpu.VMEM((fan, group, tok, hd), BF16),
        pltpu.VMEM((planes, 2, fan * tok, hd), BF16),
        pltpu.VMEM((planes, 2, fan * ctx, hd), BF16),
        pltpu.VMEM((fan, group, tok, hd), BF16),
        pltpu.VMEM((fan, group, tok, 1), F32),
        pltpu.VMEM((fan, group, tok, 1), F32),
        pltpu.VMEM((fan, group, tok, hd), F32),
        pltpu.VMEM((fan, tok, group * hd), BF16),
        pltpu.VMEM((fan, tok, group * hd), BF16),
        pltpu.VMEM((n_tp, rows, depth), BF16),
        pltpu.VMEM((n_tp, rows, depth), BF16),
        dma((2 + 2 * fan,)),
        dma((n_tp,)),
        dma((n_tp,)),
        dma((n_sp,)),
        dma((n_sp,)),
        dma((n_sp,)),
        dma((n_sp,)),
        dma((n_tp,)),
        dma((n_tp,)),
        dma((n_tp,)),
        dma((n_tp,)),
        dma((fan,)),
        dma((fan,)),
        dma((2, n_sp)),
        dma((2, n_sp)),
        dma((n_sp,)),
        dma((n_sp,)),
        dma((fan,)),
        dma((fan,)),
        dma((fan,)),
        dma((fan,)),
        dma((n_tp,)),
        dma((n_tp,)),
    ]
    return pl.pallas_call(
        functools.partial(kernel, sizes),
        out_shape=jax.ShapeDtypeStruct(latent.shape, BF16),
        in_specs=[vmem] * 11 + [hbm] * 4,
        out_specs=vmem,
        scratch_shapes=scratch,
        compiler_params=pltpu.CompilerParams(
            collective_id=0, has_side_effects=True, vmem_limit_bytes=60 * 1024 * 1024
        ),
    )(
        latent,
        condition.reshape(1, -1),
        context_condition.reshape(1, -1),
        context,
        w_shift,
        w_scale,
        w_gate,
        pre_gain.reshape(1, -1),
        post_gain.reshape(1, -1),
        query_gain.reshape(1, -1),
        key_gain.reshape(1, -1),
        w_query,
        w_key,
        w_value,
        w_out,
    )


def solution(mesh):
    placed = (
        P(("sp", "tp"), None),
        P("sp"),
        P("sp"),
        P("sp", None),
        P("sp", "tp"),
        P("sp", "tp"),
        P("sp", "tp"),
        P(),
        P(),
        P(),
        P(),
        P(None, "tp"),
        P(None, "tp"),
        P(None, "tp"),
        P("tp", None),
    )
    return jax.shard_map(
        body, mesh=mesh, in_specs=placed, out_specs=P(("sp", "tp"), None), check_vma=False
    )
```
